32 devices in a mesh: sp: 4 (over z), fs: 4 (over y, x), tp: 2 (over core).
Axes of the slice: x: 2, y: 2, z: 4, core: 2. Of those that a mesh axis runs over, the one named last changes fastest.
Arguments:
- tokens: bfloat16 [4, 8192, 2048], P('fs', 'sp'), may hold values from -21 to 21
- norm_gain: float32 [2048], replicated, may hold values from 0.1 to 1.9
- w_query: bfloat16 [2048, 1024], P(None, 'tp'), may hold values from -0.125 to 0.125
- w_key: bfloat16 [2048, 256], P(None, 'tp'), may hold values from -0.125 to 0.125
- w_value: bfloat16 [2048, 256], P(None, 'tp'), may hold values from -0.125 to 0.125
- w_pool: bfloat16 [2048, 1024], P(None, 'tp'), may hold values from -0.125 to 0.125
- w_group: bfloat16 [4, 256, 256], P('tp'), may hold values from -0.375 to 0.375
- w_out: bfloat16 [2048, 2048], replicated, may hold values from -0.125 to 0.125
- sinks: float32 [16], P('tp'), may hold values from -1 to 260
Outputs:
- mixed: bfloat16 [4, 8192, 2048], P('fs', ('sp', 'tp'))
- log_sums: float32 [4, 16, 8192], P('fs', 'tp', 'sp')
The draws below stay inside these ranges and needn't reach their ends.
All inputs are finite; a program needn't handle non-finite values.
Results may differ from the reference program's by a relative error of at most 0.009.
Values may be sent and summed in bfloat16 or wider, within the bound.
A program may use at most 192 MiB of HBM per device.

```python
import jax
import jax.numpy as jnp
from jax import lax

D = 2048
HEAD_SIZE = 64
QUERY_HEADS = 16
KEY_VALUE_HEADS = 4
GROUPS = 4
GDIM = 256
WINDOW_KEYS = 128
SEQS = 4
LEN = 8192
PW = 1024
QW = 1024
KW = 256


def draw_tokens(key, part):
    subkeys = jax.random.split(jax.random.fold_in(key, 11), 5)
    noise_part = jnp.clip(jax.random.normal(subkeys[0], (SEQS, LEN, D), jnp.float32), -4.0, 4.0)
    drift_sign = jnp.where(jax.random.uniform(subkeys[3], (SEQS, 1, 1), jnp.float32) < 0.5, -1.0, 1.0)
    drift_level = drift_sign * jax.random.uniform(subkeys[2], (SEQS, 1, 1), jnp.float32, 0.4, 1.0)
    rough_part = jax.random.uniform(subkeys[4], (SEQS, LEN // 32, 1), jnp.float32, -0.8, 0.8)
    direction = jnp.clip(jax.random.normal(subkeys[1], (SEQS, 1, D), jnp.float32), -3.0, 3.0)
    rise_factor = 1.0 + 2.0 * jnp.arange(LEN, dtype=jnp.float32)[None, :, None] / LEN
    amplitude = drift_level * rise_factor + jnp.repeat(rough_part, 32, axis=1)
    return (noise_part + amplitude * direction).astype(jnp.bfloat16)


def draw_sinks(key, part):
    subkeys = jax.random.split(jax.random.fold_in(key, 23), 1)
    sink_values = jax.random.uniform(subkeys[0], (QUERY_HEADS,), jnp.float32, -1.0, 6.0)
    return sink_values


def shard_levels(key, shape, pieces, smallest, high):
    factor_of, own = 1.0, jax.random.fold_in(key, 6)
    for position, shards_of in pieces:
        draws = jnp.exp(jax.random.uniform(jax.random.fold_in(own, position), (shards_of,), jnp.float32, smallest / len(pieces), high / len(pieces)))
        factor_of = factor_of * jnp.repeat(draws, shape[position] // shards_of).reshape([-1 if axis == position else 1 for axis in range(len(shape))])
    return factor_of


def scatter_about(stream_key, dims, width, bound, cuts=(), kind=jnp.bfloat16):
    entries = jax.random.normal(stream_key, dims, jnp.float32) * width
    if len(cuts) > 0:
        entries = shard_levels(stream_key, dims, cuts, -0.22, 0.18) * entries
    return jnp.clip(entries, min=-bound, max=bound).astype(kind)


def setup_inputs(seed: int = 0) -> dict:
    streams_of = jax.random.split(jax.random.key(seed), 10)
    return {
        "tokens": draw_tokens(jax.random.fold_in(streams_of[9], 71), 0),
        "norm_gain": jnp.clip(1.0 + 0.18 * jax.random.normal(streams_of[1], (D,), jnp.float32), 0.1, 1.9),
        "w_query": scatter_about(streams_of[2], (D, QW), D ** -0.5, 0.125, ((1, 2),)),
        "w_key": scatter_about(streams_of[3], (D, KW), D ** -0.5, 0.125, ((1, 2),)),
        "w_value": scatter_about(streams_of[4], (D, KW), D ** -0.5, 0.125, ((1, 2),)),
        "w_pool": scatter_about(streams_of[5], (D, PW), D ** -0.5, 0.125, ((1, 2),)),
        "w_group": scatter_about(streams_of[6], (GROUPS, GDIM, GDIM), GDIM ** -0.5, 0.375, ((0, 2),)),
        "w_out": scatter_about(streams_of[7], (PW + QW, D), (PW + QW) ** -0.5, 0.125),
        "sinks": draw_sinks(jax.random.fold_in(streams_of[9], 71), 0),
    }


LN_EPS = 1e-05

def normalize(token_rows, norm_gain):
    values = token_rows.astype(jnp.float32)
    row_mean = lax.optimization_barrier(jnp.mean(values, axis=-1, keepdims=True))
    centered = values - row_mean
    variance = lax.optimization_barrier(jnp.mean(centered * centered, axis=-1, keepdims=True))
    return (centered * lax.rsqrt(variance + LN_EPS) * norm_gain).astype(jnp.bfloat16)

def pool_branch(pool_rows, w_group):
    length = pool_rows.shape[0]
    reach = 2 ** GROUPS - 1
    values = pool_rows.astype(jnp.float32)
    padded = jnp.pad(values, ((reach, 0), (0, 0)))
    positions = jnp.arange(length, dtype=jnp.int32)
    prefix_mean = jnp.cumsum(values, axis=0) / (positions + 1).astype(jnp.float32)[:, None]
    outputs = []
    for group_index in range(GROUPS):
        span_width = 2 ** (group_index + 1)
        first_col = group_index * GDIM
        window_sum = jnp.zeros((length, GDIM), jnp.float32)
        for offset in range(span_width):
            window_sum = window_sum + padded[reach - offset:reach - offset + length, first_col:first_col + GDIM]
        window_count = jnp.minimum(positions + 1, span_width).astype(jnp.float32)[:, None]
        pooled = (window_sum / window_count - prefix_mean[:, first_col:first_col + GDIM]).astype(jnp.bfloat16)
        outputs.append(jnp.dot(pooled, w_group[group_index], preferred_element_type=jnp.float32).astype(jnp.bfloat16))
    return jnp.concatenate(outputs, axis=1)

def attention_branch(query_matrix, key_rows, value_rows, sinks):
    length = query_matrix.shape[0]
    block_extent = min(512, length)
    heads_per_group = QUERY_HEADS // KEY_VALUE_HEADS
    padded_keys = jnp.pad(key_rows, ((WINDOW_KEYS, 0), (0, 0)))
    padded_values = jnp.pad(value_rows, ((WINDOW_KEYS, 0), (0, 0)))
    attention_sink_logits = sinks.astype(jnp.float32).reshape(KEY_VALUE_HEADS, heads_per_group)[:, :, None, None]

    def one_block(block_index):
        start_row = (block_index * block_extent).astype(jnp.int32)
        query_tile_rows = lax.dynamic_slice_in_dim(query_matrix, start_row, block_extent, 0).reshape(block_extent, KEY_VALUE_HEADS, heads_per_group, HEAD_SIZE)
        key_tile_rows = lax.dynamic_slice_in_dim(padded_keys, start_row, block_extent + WINDOW_KEYS, 0).reshape(block_extent + WINDOW_KEYS, KEY_VALUE_HEADS, HEAD_SIZE)
        value_tile_rows = lax.dynamic_slice_in_dim(padded_values, start_row, block_extent + WINDOW_KEYS, 0).reshape(block_extent + WINDOW_KEYS, KEY_VALUE_HEADS, HEAD_SIZE)
        scores = jnp.einsum('qhrd,khd->hrqk', query_tile_rows.astype(jnp.float32), key_tile_rows.astype(jnp.float32)) * HEAD_SIZE ** (-0.5)
        query_positions = start_row + jnp.arange(block_extent, dtype=jnp.int32)
        key_positions = start_row - WINDOW_KEYS + jnp.arange(block_extent + WINDOW_KEYS, dtype=jnp.int32)
        distance = query_positions[:, None] - key_positions[None, :]
        visible = (distance >= 0) & (distance < WINDOW_KEYS) & (key_positions >= 0)[None, :]
        scores = jnp.where(visible, scores, -jnp.inf)
        row_max = jnp.maximum(lax.optimization_barrier(jnp.max(scores, axis=-1, keepdims=True)), attention_sink_logits)
        weights = jnp.exp(scores - row_max)
        weight_sum = lax.optimization_barrier(jnp.sum(weights, axis=-1, keepdims=True)) + jnp.exp(attention_sink_logits - row_max)
        normalized = (weights / weight_sum).astype(jnp.bfloat16)
        block_out = jnp.einsum('hrqk,khd->qhrd', normalized.astype(jnp.float32), value_tile_rows.astype(jnp.float32))
        block_out = block_out.astype(jnp.bfloat16).reshape(block_extent, QUERY_HEADS * HEAD_SIZE)
        block_logs = (row_max + jnp.log(weight_sum))[..., 0].reshape(QUERY_HEADS, block_extent)
        return (block_out, block_logs)
    block_outs, block_logs = lax.map(one_block, jnp.arange(length // block_extent, dtype=jnp.int32))
    attn_out = block_outs.reshape(length, QUERY_HEADS * HEAD_SIZE)
    log_sums = jnp.transpose(block_logs, (1, 0, 2)).reshape(QUERY_HEADS, length)
    return (attn_out, log_sums)

def reference(tokens, norm_gain, w_query, w_key, w_value, w_pool, w_group, w_out, sinks):

    def one_sequence(token_rows):
        normed = normalize(token_rows, norm_gain)
        query_matrix = jnp.dot(normed, w_query, preferred_element_type=jnp.float32).astype(jnp.bfloat16)
        key_rows = jnp.dot(normed, w_key, preferred_element_type=jnp.float32).astype(jnp.bfloat16)
        value_rows = jnp.dot(normed, w_value, preferred_element_type=jnp.float32).astype(jnp.bfloat16)
        pool_rows = jnp.dot(normed, w_pool, preferred_element_type=jnp.float32).astype(jnp.bfloat16)
        pool_out = pool_branch(pool_rows, w_group)
        attn_out, log_sums = attention_branch(query_matrix, key_rows, value_rows, sinks)
        joined = jnp.concatenate([pool_out, attn_out], axis=1)
        mixed = jnp.dot(joined, w_out, preferred_element_type=jnp.float32).astype(jnp.bfloat16)
        return (mixed, log_sums)
    mixed, log_sums = lax.map(one_sequence, tokens)
    return (mixed, log_sums)
```

```python
import functools

import jax
import jax.numpy as jnp
from jax import lax
from jax.experimental import pallas as pl
from jax.experimental.pallas import tpu as pltpu
from jax.sharding import PartitionSpec as P

HEAD_SIZE = 64
GDIM = 256
WINDOW = 128
LN_EPS = 1e-05
SUB = 256
HEADS = 4
HALO = 16
MESH = pl.DeviceIdType.MESH
BF = jnp.bfloat16
F32 = jnp.float32
NEG = -1e30


def dot(a, b, dims=((1,), (0,))):
    return lax.dot_general(a, b, (dims, ((), ())), preferred_element_type=F32)


def layer_kernel(
    count,
    tok_in, gain_in, wq_in, wk_in, wv_in, wp_in, wg_in, sinks_in,
    joined, logs,
    tok, gain, w, wg, sinks, norm_a, norm_b, qs, ks, vs, ps, their_attn, their_pool,
    bsum, total, totals, carry, seen_f, past_f, mixers,
    tok_sem, w_sem, small_sem, halo_send, halo_recv, sum_send, sum_recv, tp_send, tp_recv,
):
    me = lax.axis_index("sp")
    tp = lax.axis_index("tp")
    length, width = tok.shape
    tiles = length // SUB
    qw, pw, kw = wq_in.shape[1], wp_in.shape[1], wk_in.shape[1]
    groups = wg.shape[0]
    kvs = kw // HEAD_SIZE
    half_rows = length // 2
    half_blocks = half_rows // WINDOW

    def tok_copy(i):
        t = lax.rem(i + tiles - 1, tiles)
        rows = pl.ds(pl.multiple_of(t * SUB, SUB), SUB)
        return pltpu.make_async_copy(tok_in.at[rows, :], tok.at[rows, :], tok_sem.at[t])

    w_copies = [
        pltpu.make_async_copy(src, w.at[:, pl.ds(at, src.shape[1])], w_sem.at[n])
        for n, (src, at) in enumerate(
            ((wq_in, 0), (wk_in, qw), (wv_in, qw + kw), (wp_in, qw + 2 * kw))
        )
    ]
    small = [
        pltpu.make_async_copy(src, dst, small_sem.at[n])
        for n, (src, dst) in enumerate(((gain_in, gain), (wg_in, wg), (sinks_in, sinks)))
    ]
    tok_copy(0).start()
    small[0].start()
    for copy in w_copies:
        copy.start()
    tok_copy(1).start()
    small[1].start()
    small[2].start()

    totals[...] = jnp.zeros_like(totals)
    ps[: WINDOW - HALO, :] = jnp.zeros((WINDOW - HALO, pw), BF)

    @pl.when(me == 0)
    def _():
        ks[:WINDOW, :] = jnp.zeros((WINDOW, ks.shape[1]), BF)
        vs[:, :WINDOW] = jnp.zeros((vs.shape[0], WINDOW), BF)
        ps[WINDOW - HALO : WINDOW, :] = jnp.zeros((HALO, pw), BF)

    barrier = pltpu.get_barrier_semaphore()
    for hop in range(1, count):
        pl.semaphore_signal(
            barrier, inc=1, device_id={"sp": lax.rem(me + hop, count)}, device_id_type=MESH
        )
    pl.semaphore_signal(barrier, inc=1, device_id={"tp": 1 - tp}, device_id_type=MESH)

    key_id = lax.broadcasted_iota(jnp.int32, (WINDOW, 2 * WINDOW), 0)
    query_id = lax.broadcasted_iota(jnp.int32, (WINDOW, 2 * WINDOW), 1) % WINDOW
    seen_f[...] = (key_id <= query_id).astype(F32).astype(BF)
    past_f[...] = (key_id > query_id).astype(F32).astype(BF)
    drow = lax.broadcasted_iota(jnp.int32, (WINDOW, 2 * WINDOW), 0)
    dist = drow + WINDOW - lax.broadcasted_iota(jnp.int32, (WINDOW, 2 * WINDOW), 1)
    for g in range(groups):
        span = jnp.left_shift(jnp.int32(2), tp * groups + g)
        mixers[g, :WINDOW] = jnp.logical_and(dist >= 0, dist <= drow).astype(F32).astype(BF)
        mixers[g, WINDOW:] = jnp.logical_and(dist >= 0, dist < span).astype(F32).astype(BF)

    def norm_rows(dst, base, r0, rows):
        x = tok[pl.ds(pl.multiple_of(base + r0, rows), rows), :].astype(F32)
        centered = x - jnp.sum(x, axis=-1, keepdims=True) * (1.0 / width)
        variance = jnp.sum(centered * centered, axis=-1, keepdims=True) * (1.0 / width)
        dst[r0 : r0 + rows, :] = (
            centered * lax.rsqrt(variance + LN_EPS) * gain[...]
        ).astype(BF)

    def project_tile(i, src, dst):
        t = lax.rem(i + tiles - 1, tiles)
        base = pl.multiple_of(t * SUB, SUB)
        nxt = pl.multiple_of(lax.rem(i + tiles, tiles) * SUB, SUB)
        rows = pl.ds(base, SUB)
        shifted = pl.ds(base + WINDOW, SUB)
        chunk = 16
        todo = [functools.partial(norm_rows, dst, nxt, r0, chunk) for r0 in range(0, SUB, chunk)]

        def norms(n):
            for _ in range(min(n, len(todo))):
                todo.pop(0)()

        x = src[...]
        norms(3)
        qs[rows, :] = (dot(x, w[:, :qw]) * HEAD_SIZE**-0.5).astype(BF)
        norms(5)
        kv = dot(x, w[:, qw : qw + 2 * kw])
        norms(3)
        p = dot(x, w[:, qw + 2 * kw :]).astype(BF)
        norms(16)
        k = kv[:, :kw]
        lane = lax.broadcasted_iota(jnp.int32, k.shape, 1)
        low = lane < HEAD_SIZE
        rolled = pltpu.roll(k, HEAD_SIZE, 1)
        zero = jnp.zeros_like(k)
        for n, part in enumerate(
            (
                jnp.where(low, k, zero), jnp.where(low, zero, rolled),
                jnp.where(low, rolled, zero), jnp.where(low, zero, k),
            )
        ):
            ks[shifted, n * WINDOW : (n + 1) * WINDOW] = part.astype(BF)
        vs[:, shifted] = kv[:, kw:].T.astype(BF)
        ps[shifted, :] = p
        pf = p.astype(F32)
        for b in range(SUB // WINDOW):
            part = jnp.sum(
                pf[b * WINDOW : (b + 1) * WINDOW].reshape(WINDOW // 8, 8, pw), axis=0
            )
            bsum[t * (SUB // WINDOW) + b] = part

    halo_pairs = (
        (ks.at[pl.ds(length, WINDOW), :], ks.at[pl.ds(0, WINDOW), :]),
        (vs.at[:, pl.ds(length, WINDOW)], vs.at[:, pl.ds(0, WINDOW)]),
        (
            ps.at[pl.ds(length + WINDOW - HALO, HALO), :],
            ps.at[pl.ds(WINDOW - HALO, HALO), :],
        ),
    )
    halos = [
        pltpu.make_async_remote_copy(
            src_ref=src, dst_ref=dst, send_sem=halo_send.at[n], recv_sem=halo_recv.at[n],
            device_id={"sp": lax.rem(me + 1, count)}, device_id_type=MESH,
        )
        for n, (src, dst) in enumerate(halo_pairs)
    ]

    def sum_copy(hop):
        return pltpu.make_async_remote_copy(
            src_ref=total, dst_ref=totals.at[hop], send_sem=sum_send.at[hop],
            recv_sem=sum_recv.at[hop], device_id={"sp": lax.rem(me + hop, count)},
            device_id_type=MESH,
        )

    tok_copy(0).wait()
    small[0].wait()
    for r0 in range(0, SUB, 16):
        norm_rows(norm_a, (tiles - 1) * SUB, r0, 16)
    for copy in w_copies:
        copy.wait()

    def project_pair(j, _):
        i = 2 * j

        @pl.when(j == 1)
        def _():
            pl.semaphore_wait(barrier, count)

            @pl.when(me < count - 1)
            def _():
                for copy in halos:
                    copy.start()

        tok_copy(i + 1).wait()

        @pl.when(i + 2 < tiles)
        def _():
            tok_copy(i + 2).start()
            tok_copy(i + 3).start()

        project_tile(i, norm_a, norm_b)

        @pl.when(i + 2 < tiles)
        def _():
            tok_copy(i + 2).wait()

        project_tile(i + 1, norm_b, norm_a)
        return 0

    lax.fori_loop(0, tiles // 2, project_pair, 0)

    acc = bsum[0]
    for b in range(1, length // WINDOW):
        acc = acc + bsum[b]
    total[...] = acc

    small[1].wait()
    small[2].wait()

    @pl.when(me > 0)
    def _():
        for copy in halos:
            copy.wait_recv()

    @pl.when(me < count - 1)
    def _():
        for copy in halos:
            copy.wait_send()

    for hop in range(1, count):

        @pl.when(me + hop < count)
        def _():
            sum_copy(hop).start()

    def score(block, kv):
        start = pl.multiple_of(block * WINDOW, WINDOW)
        window = pl.ds(start, 2 * WINDOW)
        c = kv * 2 * WINDOW
        rhs = jnp.concatenate(
            [qs[pl.ds(start, WINDOW), c + n * WINDOW : c + (n + 1) * WINDOW] for n in range(2)],
            axis=0,
        )
        lhs = jnp.concatenate(
            [ks[window, c + n * WINDOW : c + (n + 1) * WINDOW] for n in range(2)], axis=0
        )
        return dot(lhs, rhs, ((1,), (1,)))

    def attend(block, kv, scores, penalty):
        cols = pl.ds(pl.multiple_of(block * WINDOW, WINDOW), WINDOW)
        seen = seen_f[...] > 0
        stacked, scales = [], []
        for parity in range(2):
            s = scores[parity * 2 * WINDOW : (parity + 1) * 2 * WINDOW]
            past = s[:WINDOW]
            if penalty is not None:
                past = past + penalty
            picked = jnp.where(seen, s[WINDOW:], past)
            heads = [kv * HEADS + 2 * pair + parity for pair in range(2)]
            sink = jnp.concatenate(
                [jnp.full((1, WINDOW), sinks[h], F32) for h in heads], axis=1
            )
            row_max = jnp.maximum(jnp.max(picked, axis=0, keepdims=True), sink)
            weights = jnp.exp(picked - row_max)
            weight_sum = jnp.sum(weights, axis=0, keepdims=True) + jnp.exp(sink - row_max)
            log_row = row_max + jnp.log(weight_sum)
            for pair in range(2):
                logs[heads[pair] : heads[pair] + 1, cols] = log_row[
                    :, pair * WINDOW : (pair + 1) * WINDOW
                ]
            wb = weights.astype(BF)
            stacked.append(jnp.concatenate([wb * past_f[...], wb * seen_f[...]], axis=0))
            scales.append(1.0 / weight_sum)
        return stacked, scales

    def collect(block, kv, stacked, scales, dest, row, col):
        window = pl.ds(pl.multiple_of(block * WINDOW, WINDOW), 2 * WINDOW)
        v = vs[kv * HEAD_SIZE : (kv + 1) * HEAD_SIZE, window]
        outs = [dot(v, s) * scale for s, scale in zip(stacked, scales)]
        for pair in range(2):
            cols = slice(pair * WINDOW, (pair + 1) * WINDOW)
            o = jnp.concatenate([o[:, cols] for o in outs], axis=0)
            at = col + (kv * 2 + pair) * WINDOW
            if not isinstance(at, int):
                at = pl.multiple_of(at, WINDOW)
            dest[pl.ds(row, WINDOW), pl.ds(at, WINDOW)] = o.astype(BF).T

    def pool_block(block, g, dest, row, col):
        start = pl.multiple_of(block * WINDOW, WINDOW)
        cols = slice(g * GDIM, (g + 1) * GDIM)
        position = (
            me * length + block * WINDOW + 1
            + lax.broadcasted_iota(jnp.int32, (WINDOW, WINDOW), 0)
        )
        span = jnp.left_shift(jnp.int32(2), tp * groups + g)
        inv_pos = 1.0 / position.astype(F32)
        inv_count = 1.0 / jnp.minimum(position, span).astype(F32)
        inv_pos = jnp.concatenate([inv_pos] * (GDIM // WINDOW), axis=1)
        inv_count = jnp.concatenate([inv_count] * (GDIM // WINDOW), axis=1)
        sums = dot(mixers[g], ps[pl.ds(start, 2 * WINDOW), cols])
        before = carry[pl.ds(block, 1), cols]
        pooled = (sums[WINDOW:] * inv_count - (sums[:WINDOW] + before) * inv_pos).astype(BF)
        at = col + g * GDIM
        if not isinstance(at, int):
            at = pl.multiple_of(at, GDIM)
        dest[pl.ds(row, WINDOW), pl.ds(at, GDIM)] = dot(pooled, wg[g]).astype(BF)

    def mix(first, blocks, attn_to, pools):
        dest, row0, col = attn_to
        units = [(b, kv) for b in range(blocks) for kv in range(kvs)]
        nopast = jnp.logical_and(first == 0, me == 0)
        penalty = jnp.where(nopast, F32(NEG), F32(0))
        per = -(-len(pools) // len(units)) if units else 0
        pools = list(pools)

        def where(b):
            return pl.multiple_of(row0 + b * WINDOW, WINDOW)

        scores = score(first + units[0][0], units[0][1])
        pending = None
        for u, (b, kv) in enumerate(units):
            later = None
            if u + 1 < len(units):
                later = score(first + units[u + 1][0], units[u + 1][1])
            if pending is not None:
                collect(*pending)
            for _ in range(min(per, len(pools))):
                pool_block(*pools.pop(0))
            done = attend(first + b, kv, scores, penalty if b == 0 else None)
            pending = (first + b, kv, *done, dest, where(b), col)
            scores = later
        collect(*pending)

    mine, other = tp * half_blocks, (1 - tp) * half_blocks
    step = half_blocks // 2
    attn_col = 2 * pw + tp * qw
    pool_col = tp * pw

    def their_step(j, _):
        mix(other + j * step, step, (their_attn, j * step * WINDOW, 0), ())
        return 0

    lax.fori_loop(0, 2, their_step, 0)

    def tp_copy(n):
        src, col = ((their_attn, attn_col), (their_pool, pool_col))[n]
        return pltpu.make_async_remote_copy(
            src_ref=src,
            dst_ref=joined.at[:, pl.ds(pl.multiple_of(col, 512), src.shape[1])],
            send_sem=tp_send.at[n], recv_sem=tp_recv.at[n],
            device_id={"tp": 1 - tp}, device_id_type=MESH,
        )

    for hop in range(1, count):

        @pl.when(me >= hop)
        def _():
            sum_copy(hop).wait_recv()

        @pl.when(me + hop < count)
        def _():
            sum_copy(hop).wait_send()

    tp_copy(0).start()
    acc = jnp.sum(totals[...], axis=0)
    for b in range(length // WINDOW):
        carry[b : b + 1, :] = jnp.sum(acc, axis=0, keepdims=True)
        acc = acc + bsum[b]

    mix(
        mine, step, (joined, 0, attn_col),
        [(other + b, g, their_pool, b * WINDOW, 0) for b in range(half_blocks) for g in range(groups)],
    )
    tp_copy(1).start()
    mix(
        mine + step, step, (joined, step * WINDOW, attn_col),
        [(mine + b, g, joined, b * WINDOW, pool_col) for b in range(half_blocks) for g in range(groups)],
    )

    for n in range(2):
        src, col = ((their_attn, 2 * pw + (1 - tp) * qw), (their_pool, (1 - tp) * pw))[n]
        tp_copy(n).wait_send()
        tp_copy(n).wait_recv()


def layer(tokens, gain, wq, wk, wv, wp, wg, sinks):
    length, width = tokens.shape
    count = lax.axis_size("sp")
    qw, kw, pw = wq.shape[1], wk.shape[1], wp.shape[1]
    groups = wg.shape[0]
    blocks = length // WINDOW
    heads = sinks.shape[0]
    any_ = pl.BlockSpec(memory_space=pl.ANY)
    vmem = pl.BlockSpec(memory_space=pltpu.VMEM)
    return pl.pallas_call(
        functools.partial(layer_kernel, count),
        in_specs=[any_] * 8,
        out_specs=[vmem, vmem],
        out_shape=[
            pltpu.VMEM((length // 2, 2 * (qw + pw)), BF),
            pltpu.VMEM((heads, length), F32),
        ],
        scratch_shapes=[
            pltpu.VMEM((length, width), BF),
            pltpu.VMEM(gain.shape, F32),
            pltpu.VMEM((width, qw + 2 * kw + pw), BF),
            pltpu.VMEM(wg.shape, BF),
            pltpu.SMEM(sinks.shape, F32),
            pltpu.VMEM((SUB, width), BF),
            pltpu.VMEM((SUB, width), BF),
            pltpu.VMEM((length, qw), BF),
            pltpu.VMEM((length + WINDOW, 4 * kw), BF),
            pltpu.VMEM((kw, length + WINDOW), BF),
            pltpu.VMEM((length + WINDOW, pw), BF),
            pltpu.VMEM((length // 2, qw), BF),
            pltpu.VMEM((length // 2, pw), BF),
            pltpu.VMEM((blocks, 8, pw), F32),
            pltpu.VMEM((8, pw), F32),
            pltpu.VMEM((count, 8, pw), F32),
            pltpu.VMEM((blocks, pw), F32),
            pltpu.VMEM((WINDOW, 2 * WINDOW), BF),
            pltpu.VMEM((WINDOW, 2 * WINDOW), BF),
            pltpu.VMEM((groups, 2 * WINDOW, 2 * WINDOW), BF),
            pltpu.SemaphoreType.DMA((length // SUB,)),
            pltpu.SemaphoreType.DMA((4,)),
            pltpu.SemaphoreType.DMA((3,)),
            pltpu.SemaphoreType.DMA((3,)),
            pltpu.SemaphoreType.DMA((3,)),
            pltpu.SemaphoreType.DMA((count,)),
            pltpu.SemaphoreType.DMA((count,)),
            pltpu.SemaphoreType.DMA((2,)),
            pltpu.SemaphoreType.DMA((2,)),
        ],
        compiler_params=pltpu.CompilerParams(
            collective_id=0, has_side_effects=True, vmem_limit_bytes=40 * 2**20
        ),
        cost_estimate=pl.CostEstimate(
            flops=2 * length * width * (qw + 2 * kw + pw),
            bytes_accessed=2 * length * width, transcendentals=0,
        ),
        name="layer",
    )(tokens, gain, wq, wk, wv, wp, wg, sinks)


def output_kernel(joined, logs_in, w, out, logs):
    @pl.when(pl.program_id(0) == 0)
    def _():
        logs[...] = logs_in[...]

    out[...] = dot(joined[...], w[...]).astype(BF)


def output(joined, logs, w):
    rows = joined.shape[0]
    depth, cols = w.shape
    tile = 256
    vmem = pl.BlockSpec(memory_space=pltpu.VMEM)
    return pl.pallas_call(
        output_kernel,
        grid=(cols // tile,),
        in_specs=[
            vmem,
            vmem,
            pl.BlockSpec((depth, tile), lambda i: (0, i)),
        ],
        out_specs=[
            pl.BlockSpec((rows, tile), lambda i: (0, i)),
            pl.BlockSpec(logs.shape, lambda i: (0, 0)),
        ],
        out_shape=[
            jax.ShapeDtypeStruct((rows, cols), BF),
            jax.ShapeDtypeStruct(logs.shape, F32),
        ],
        compiler_params=pltpu.CompilerParams(
            dimension_semantics=("arbitrary",), vmem_limit_bytes=40 * 2**20
        ),
        cost_estimate=pl.CostEstimate(
            flops=2 * rows * depth * cols, bytes_accessed=2 * w.size, transcendentals=0
        ),
        name="output",
    )(joined, logs, w)


def body(tokens, norm_gain, w_query, w_key, w_value, w_pool, w_group, w_out, sinks):
    joined, logs = layer(
        tokens[0], norm_gain[None, :], w_query, w_key, w_value, w_pool, w_group, sinks
    )
    mixed, logs = output(joined, logs, w_out)
    return (mixed[None], logs[None])


def solution(mesh):
    return jax.shard_map(
        body,
        mesh=mesh,
        in_specs=(
            P("fs", "sp", None),
            P(),
            P(None, "tp"),
            P(None, "tp"),
            P(None, "tp"),
            P(None, "tp"),
            P("tp", None, None),
            P(),
            P("tp"),
        ),
        out_specs=(P("fs", ("sp", "tp"), None), P("fs", "tp", "sp")),
        check_vma=False,
    )
```
